512 devices in a mesh: fs: 128 (over z, y, core), tp: 4 (over x).
Axes of the slice: x: 4, y: 8, z: 8, core: 2. Of those that a mesh axis runs over, the one named last changes fastest.
Arguments:
- inputs: bfloat16 [73728, 2048], P('fs'), may hold values from -24 to 24
- query_cotangent: bfloat16 [73728, 1024], P('fs', 'tp'), may hold values from -0.017944336 to 0.017944336
- value_cotangent: bfloat16 [73728, 1024], P('fs', 'tp'), may hold values from -0.017944336 to 0.017944336
- weights_query: float32 [2048, 1024], P('fs', 'tp'), may hold values from -6 to 6
- weights_value: float32 [2048, 1024], P('fs', 'tp'), may hold values from -6 to 6
- basis_query: bfloat16 [1024, 32], P('tp'), may hold values from -0.75 to 0.75
- basis_value: bfloat16 [1024, 32], P('tp'), may hold values from -0.75 to 0.75
- first_query: float32 [2048, 512], P('fs', 'tp'), may hold values from -5.4 to 5.4, as said below
- second_query: float32 [2048, 512], P('fs', 'tp'), may hold values from 0.05 to 1
- first_value: float32 [2048, 512], P('fs', 'tp'), may hold values from -5.4 to 5.4, as said below
- second_value: float32 [2048, 512], P('fs', 'tp'), may hold values from 0.05 to 1
Outputs:
- step_query: float32 [2048, 1024], P('fs', 'tp')
- step_value: float32 [2048, 1024], P('fs', 'tp')
- new_query: float32 [2048, 1024], P('fs', 'tp')
- new_value: float32 [2048, 1024], P('fs', 'tp')
- copy_query: bfloat16 [2048, 1024], P(None, 'tp')
- copy_value: bfloat16 [2048, 1024], P(None, 'tp')
- moment_query: float32 [2048, 512], P('fs', 'tp')
- square_query: float32 [2048, 512], P('fs', 'tp')
- moment_value: float32 [2048, 512], P('fs', 'tp')
- square_value: float32 [2048, 512], P('fs', 'tp')
The draws below stay inside these ranges and needn't reach their ends.
Inputs may be any that keep to these rules, and one draw needn't show every extreme that they name: `first_query`: first moments, with a spread of scale from row to row. `first_value`: first moments, with a spread of scale from row to row.
All inputs are finite; a program needn't handle non-finite values.
Results may differ from the reference program's by a relative error of at most 0.003.
Values may be sent and summed in bfloat16 or wider, within the bound.
A program may use at most 64 MiB of HBM per device.

```python
import math
import jax
import jax.numpy as jnp
from jax import lax

D = 2048
HEADS = 16
HEAD = 64
RK = 32
FW = 1024
TOKENS = 73728


def moment_draw(key):
    base = 0.3 * jnp.clip(jax.random.normal(jax.random.fold_in(key, 11), (D, HEADS * RK), jnp.float32), -4.0, 4.0)
    factor = jnp.exp(jax.random.uniform(jax.random.fold_in(key, 12), (D, 1), jnp.float32, -1.5, 1.5))
    return base * factor


def draw_first_query(key, part):
    return moment_draw(jax.random.fold_in(key, 1))


def draw_first_value(key, part):
    return moment_draw(jax.random.fold_in(key, 2))


def raised(drawn, own_key, source, target, parts, factor):
    owner, partner = [(jnp.arange(drawn.shape[position]) // (drawn.shape[position] // parts)).reshape([-1 if axis == position else 1 for axis in range(drawn.ndim)]) for position in (source, target)]
    chosen = jax.random.permutation(own_key, parts)[partner]
    strong = (owner == chosen) | (owner == (partner + parts // 2) % parts)
    return jnp.where(strong, factor * drawn, drawn)


def block_levels(rng, shape, cuts, smallest, high):
    level, own = 1.0, jax.random.fold_in(rng, 6)
    for axis_at, shards_of in cuts:
        heights = jnp.exp(jax.random.uniform(jax.random.fold_in(own, axis_at), (shards_of,), jnp.float32, smallest / len(cuts), high / len(cuts)))
        level = level * jnp.repeat(heights, shape[axis_at] // shards_of).reshape([-1 if axis == axis_at else 1 for axis in range(len(shape))])
    return level


def bell_draw(rng, dims, width, bound, cuts=(), held_as=jnp.bfloat16):
    entries = jax.random.normal(rng, dims, jnp.float32) * width
    if len(cuts) > 0:
        entries = block_levels(rng, dims, cuts, -0.22, 0.18) * entries
    return jnp.clip(entries, min=-bound, max=bound).astype(held_as)


def bell_draw_with(rng, extent, width, most, cuts, heavy, dtype=jnp.bfloat16):
    drawn = width * jax.random.normal(rng, extent, jnp.float32)
    if cuts:
        drawn = drawn * block_levels(rng, extent, cuts, -0.22, 0.18)
    return jnp.clip(raised(drawn, jax.random.fold_in(rng, 3), *heavy), -most, most).astype(dtype)


def setup_inputs(seed: int = 0) -> dict:
    key_list = jax.random.split(jax.random.key(seed), 12)
    inputs = bell_draw_with(key_list[0], (TOKENS, D), 1.0, 24.0, ((0, 128),), (0, 1, 128, 5.5))
    query_cotangent = bell_draw(key_list[1], (TOKENS, FW), 0.003, 0.017944336, ((0, 128), (1, 4)))
    value_cotangent = bell_draw(key_list[2], (TOKENS, FW), 0.003, 0.017944336, ((0, 128), (1, 4)))
    weights_query = bell_draw(key_list[3], (D, FW), 1.0, 6.0, ((0, 128), (1, 4)), jnp.float32)
    weights_value = bell_draw(key_list[4], (D, FW), 1.0, 6.0, ((0, 128), (1, 4)), jnp.float32)
    basis_query = bell_draw(key_list[5], (FW, RK), HEAD ** -0.5, 0.75, ((0, 4),))
    basis_value = bell_draw(key_list[6], (FW, RK), HEAD ** -0.5, 0.75, ((0, 4),))
    first_query = draw_first_query(jax.random.fold_in(key_list[11], 71), 0)
    second_query = jnp.clip(jnp.exp(math.log(1.0) - 2.9957323 * jax.random.uniform(key_list[8], (D, HEADS * RK), jnp.float32) ** block_levels(key_list[8], (D, HEADS * RK), ((0, 128), (1, 4)), -0.2, 0.2)), 0.05, 1.0)
    first_value = draw_first_value(jax.random.fold_in(key_list[11], 71), 0)
    second_value = jnp.clip(jnp.exp(math.log(1.0) - 2.9957323 * jax.random.uniform(key_list[10], (D, HEADS * RK), jnp.float32) ** block_levels(key_list[10], (D, HEADS * RK), ((0, 128), (1, 4)), -0.2, 0.2)), 0.05, 1.0)
    return {"inputs": inputs, "query_cotangent": query_cotangent, "value_cotangent": value_cotangent, "weights_query": weights_query, "weights_value": weights_value, "basis_query": basis_query, "basis_value": basis_value, "first_query": first_query, "second_query": second_query, "first_value": first_value, "second_value": second_value}


def apply_basis(gradient, basis):
    split = gradient.reshape(D, HEADS, HEAD)
    factor = basis.reshape(HEADS, HEAD, RK).astype(jnp.float32)
    out = jnp.einsum('nhd,hdr->nhr', split, factor, precision=lax.Precision.HIGHEST)
    return out.reshape(D, HEADS * RK)

def expand(direction, basis):
    split = direction.reshape(D, HEADS, RK)
    factor = basis.reshape(HEADS, HEAD, RK).astype(jnp.float32)
    out = jnp.einsum('nhr,hdr->nhd', split, factor, precision=lax.Precision.HIGHEST)
    return out.reshape(D, HEADS * HEAD)

def update(inputs, cotangent, weights, basis, first, second):
    gradient = jnp.dot(inputs.T, cotangent, preferred_element_type=jnp.float32)
    reduced = apply_basis(gradient, basis)
    moment = 0.9 * first + 0.1 * reduced
    square = 0.95 * second + 0.05 * reduced * reduced
    direction = moment / (jnp.sqrt(square) + 1e-08)
    scale = 1.0 / jnp.sqrt(jnp.mean(direction * direction) + 0.25)
    step = scale * expand(direction, basis)
    fresh = weights - 0.1 * step
    return (step, fresh, fresh.astype(jnp.bfloat16), moment, square)

def reference(inputs, query_cotangent, value_cotangent, weights_query, weights_value, basis_query, basis_value, first_query, second_query, first_value, second_value):
    step_q, new_q, copy_q, moment_q, square_q = update(inputs, query_cotangent, weights_query, basis_query, first_query, second_query)
    step_v, new_v, copy_v, moment_v, square_v = update(inputs, value_cotangent, weights_value, basis_value, first_value, second_value)
    return (step_q, step_v, new_q, new_v, copy_q, copy_v, moment_q, square_q, moment_v, square_v)
```

```python
import functools

import jax
import jax.numpy as jnp
from jax import lax
from jax.experimental import pallas as pl
from jax.experimental.pallas import tpu as pltpu
from jax.sharding import PartitionSpec as P

D = 2048
HEADS = 16
HEAD = 64
RK = 32
N = 8
ORDER = (4, 3, 5, 2, 6, 1, 7)
BF = jnp.bfloat16
F32 = jnp.float32
MESH = pl.DeviceIdType.MESH
ANY = pl.BlockSpec(memory_space=pl.ANY)
VM = pl.BlockSpec(memory_space=pltpu.VMEM)


def spread(basis):
    rows, rank = basis.shape
    heads = rows // HEAD
    wide = heads * rank
    copies = lax.broadcasted_iota(jnp.int32, (rank, wide), 1) % rank
    pick = (lax.broadcasted_iota(jnp.int32, (rank, wide), 0) == copies).astype(BF)
    tiled = jnp.dot(basis, pick, preferred_element_type=F32)
    row = lax.broadcasted_iota(jnp.int32, (rows, wide), 0) // HEAD
    col = lax.broadcasted_iota(jnp.int32, (rows, wide), 1) // rank
    return jnp.where(row == col, tiled, 0.0).astype(BF)


def moments(reduced, first, second):
    moment = 0.9 * first + 0.1 * reduced
    square = 0.95 * second + 0.05 * reduced * reduced
    direction = moment / (jnp.sqrt(square) + 1e-08)
    return moment, square, direction


def encode(w):
    s = w * w
    return jnp.where(w < 0, -(s * s), s * s).astype(BF)


def decode(code):
    c = code.astype(F32)
    size = lax.rsqrt(lax.rsqrt(jnp.maximum(jnp.abs(c), 1e-30)))
    return jnp.where(c < 0, -size, size)


def talk(
    x_hbm, qc_hbm, vc_hbm, bq_hbm, bv_hbm, wq_hbm, wv_hbm, fq_hbm, sq_hbm, fv_hbm, sv_hbm,
    dq_out, dv_out, wq_out, wv_out, red_out, ss_out,
    x, qc, vc, bq, bv, wq, wv, mom, small, mine, d2d_send, d2d_recv,
    send_q, recv_q, send_v, recv_v, send2_q, recv2_q, send2_v, recv2_v,
    dq, dv, wall_q, wall_v, red, ss, load_sem, ssem, rsem,
):
    fs = lax.axis_index("fs")
    tp = lax.axis_index("tp")
    c = fs % 2
    y = (fs // 2) % N
    z = fs // (2 * N)
    other = fs + 1 - 2 * c

    def on_y(k):
        return {"fs": (z * N + (y + k) % N) * 2 + c}

    def on_z(k):
        return {"fs": (((z + k) % N) * N + y) * 2 + c}

    partner = {"fs": other}
    over_x = [{"fs": f, "tp": (tp + k) % 4} for f, k in
              [(fs, 1), (fs, 2), (fs, 3), (other, 0), (other, 1), (other, 2), (other, 3)]]

    barrier = pltpu.get_barrier_semaphore()
    greeted = [on_y(k) for k in ORDER] + [on_z(k) for k in ORDER] + over_x
    for device in greeted:
        pl.semaphore_signal(barrier, inc=1, device_id=device, device_id_type=MESH)

    loads = []

    def load(src, dst):
        copy = pltpu.make_async_copy(src, dst, load_sem.at[len(loads)])
        copy.start()
        loads.append(copy)
        return copy

    sent = []

    def send(src, dst, device):
        at = len(sent)
        copy = pltpu.make_async_remote_copy(
            src_ref=src, dst_ref=dst, send_sem=ssem.at[at], recv_sem=rsem.at[at],
            device_id=device, device_id_type=MESH)
        copy.start()
        sent.append(copy)
        return copy

    first = [load(bq_hbm, bq), load(bv_hbm, bv), load(qc_hbm, qc), load(vc_hbm, vc)]
    order = ORDER + (0,)
    chunk_z = [(z + k) % N for k in order]
    chunks = [
        load(x_hbm.at[:, pl.ds(pl.multiple_of(chunk_z[j] * 256, 256), 256)], x.at[j]) for j in range(N)
    ]
    later_w = [load(wq_hbm, wq), load(wv_hbm, wv)]
    later_m = [load(r, mom.at[i]) for i, r in enumerate((fq_hbm, sq_hbm, fv_hbm, sv_hbm))]

    for copy in first:
        copy.wait()
    small[:, :128] = jnp.dot(qc[...], spread(bq[...]), preferred_element_type=F32).astype(BF)
    small[:, 128:] = jnp.dot(vc[...], spread(bv[...]), preferred_element_type=F32).astype(BF)

    d2d = []

    def product(j):
        chunks[j].wait()
        out = lax.dot_general(x[j], small[...], (((0,), (0,)), ((), ())), preferred_element_type=F32)
        out = out.reshape(N, 2, 16, 256)
        p0, p1 = out[:, 0], out[:, 1]
        own = jnp.where(c == 0, p0, p1)
        away = jnp.where(c == 0, p1, p0).astype(BF)
        mine[j, 0] = own[:, :, :128]
        mine[j, 1] = own[:, :, 128:]
        d2d_send[j, 0] = away[:, :, :128]
        d2d_send[j, 1] = away[:, :, 128:]

    rs1_v = []

    def combine(j):
        d2d[j].wait_recv()
        send_q[:, pl.ds(chunk_z[j], 1)] = (mine[j, 0] + d2d_recv[j, 0].astype(F32)).astype(BF)[:, None]
        send_v[j] = (mine[j, 1] + d2d_recv[j, 1].astype(F32)).astype(BF)
        if order[j] != 0:
            rs1_v.append((order[j], send(send_v.at[j], recv_v.at[order[j]], on_z(order[j]))))

    product(0)
    pl.semaphore_wait(barrier, len(greeted))

    for copy in later_w:
        copy.wait()
    wall_q[pl.ds(c, 1), pl.ds(y, 1), pl.ds(z, 1)] = encode(wq[...])[None, None, None]
    wall_v[pl.ds(c, 1), pl.ds(z, 1), pl.ds(y, 1)] = encode(wv[...])[None, None, None]
    d2d.append(send(d2d_send.at[0], d2d_recv.at[0], partner))
    w1 = []
    for k in ORDER:
        w1.append(send(wall_q.at[c, y, z], wall_q.at[c, y, z], on_z(k)))
        w1.append(send(wall_v.at[c, z, y], wall_v.at[c, z, y], on_y(k)))
    for j in range(1, N):
        product(j)
        d2d.append(send(d2d_send.at[j], d2d_recv.at[j], partner))
        combine(j - 1)
    combine(N - 1)
    rs1_q = [(k, send(send_q.at[(y + k) % N], recv_q.at[k], on_y(k))) for k in ORDER]

    forwards = []

    def forward(ref, index):
        forwards.append(send(ref.at[c, index], ref.at[c, index], partner))

    for copy in w1:
        copy.wait_recv()
    right, left = [], []

    def w_step(s):
        if s > 0:
            right[-2].wait_recv()
            right[-1].wait_recv()
            forward(wall_q, (y + N - s) % N)
            forward(wall_v, (z + N - s) % N)
            if s < 4:
                left[-2].wait_recv()
                left[-1].wait_recv()
                forward(wall_q, (y + s) % N)
                forward(wall_v, (z + s) % N)
        else:
            forward(wall_q, y)
            forward(wall_v, z)
        if s < 4:
            a, b = (y + N - s) % N, (z + N - s) % N
            right.append(send(wall_q.at[c, a], wall_q.at[c, a], on_y(1)))
            right.append(send(wall_v.at[c, b], wall_v.at[c, b], on_z(1)))
        if s < 3:
            a, b = (y + s) % N, (z + s) % N
            left.append(send(wall_q.at[c, a], wall_q.at[c, a], on_y(N - 1)))
            left.append(send(wall_v.at[c, b], wall_v.at[c, b], on_z(N - 1)))

    w_step(0)

    total_v = send_v[N - 1].astype(F32)
    for k, copy in rs1_v:
        copy.wait_recv()
        total_v = total_v + recv_v[k].astype(F32)
    send2_v[...] = total_v.astype(BF)
    rs2_v = [(k, send(send2_v.at[(y + k) % N], recv2_v.at[k], on_y(k))) for k in ORDER]
    total_q = send_q[pl.ds(y, 1)][0].astype(F32)
    for k, copy in rs1_q:
        copy.wait_recv()
        total_q = total_q + recv_q[k].astype(F32)
    send2_q[...] = total_q.astype(BF)
    rs2_q = [(k, send(send2_q.at[(z + k) % N], recv2_q.at[k], on_z(k))) for k in ORDER]
    w_step(1)

    reduced_v = send2_v[pl.ds(y, 1)][0].astype(F32)
    for k, copy in rs2_v:
        copy.wait_recv()
        reduced_v = reduced_v + recv2_v[k].astype(F32)
    reduced_q = send2_q[pl.ds(z, 1)][0].astype(F32)
    for k, copy in rs2_q:
        copy.wait_recv()
        reduced_q = reduced_q + recv2_q[k].astype(F32)
    for copy in later_m:
        copy.wait()
    red[0] = reduced_q
    red[1] = reduced_v
    direction_q = moments(reduced_q, mom[0], mom[1])[2]
    direction_v = moments(reduced_v, mom[2], mom[3])[2]
    dq[pl.ds(c, 1), pl.ds(y, 1), pl.ds(z, 1)] = direction_q.astype(BF)[None, None, None]
    dv[pl.ds(c, 1), pl.ds(z, 1), pl.ds(y, 1)] = direction_v.astype(BF)[None, None, None]
    ag1 = []
    for k in ORDER:
        ag1.append(send(dq.at[c, y, z], dq.at[c, y, z], on_z(k)))
        ag1.append(send(dv.at[c, z, y], dv.at[c, z, y], on_y(k)))
    w_step(2)
    for copy in ag1:
        copy.wait_recv()
    ag2 = []
    for k in ORDER:
        ag2.append((k, send(dq.at[c, y], dq.at[c, y], on_y(k)), send(dv.at[c, z], dv.at[c, z], on_z(k))))
    forward(dq, y)
    forward(dv, z)
    w_step(3)

    def squares(ref, index):
        t = ref[pl.ds(c, 1), pl.ds(index, 1)].astype(F32).reshape(N * 2, 8, 128)
        return jnp.sum(t * t, axis=0)

    ss_q = squares(dq, y)
    ss_v = squares(dv, z)
    for k, copy_q, copy_v in sorted(ag2, key=lambda t: min(t[0], N - t[0])):
        a, b = (y + N - k) % N, (z + N - k) % N
        copy_q.wait_recv()
        forward(dq, a)
        ss_q = ss_q + squares(dq, a)
        copy_v.wait_recv()
        forward(dv, b)
        ss_v = ss_v + squares(dv, b)
    ss[0, 0] = ss_q
    ss[0, 1] = ss_v
    sums = [send(ss.at[0], ss.at[1 + i], device) for i, device in enumerate(over_x)]
    w_step(4)
    for copy in forwards:
        copy.wait_recv()
    at = len(loads)
    outs = [load(dq, dq_out), load(dv, dv_out), load(wall_q, wq_out), load(wall_v, wv_out), load(red, red_out)]
    for copy in sums:
        copy.wait_recv()
    outs.append(load(ss, ss_out))
    for copy in sent:
        copy.wait_send()
    for copy in outs:
        copy.wait()


def finish(
    dq, dv, wall_q, wall_v, red, ss, bq, bv, wq, wv, fq, sq, fv, sv,
    step_q, step_v, new_q, new_v, copy_q, copy_v, moment_q, square_q, moment_v, square_v,
):
    entries = D * HEADS * RK
    sums = jnp.sum(ss[...], axis=0)
    turn = (((1,), (1,)), ((), ()))
    for which, (d, wall, b, w, f, s, step, new, copy, moment, square) in enumerate((
        (dq, wall_q, bq, wq, fq, sq, step_q, new_q, copy_q, moment_q, square_q),
        (dv, wall_v, bv, wv, fv, sv, step_v, new_v, copy_v, moment_v, square_v),
    )):
        factor = spread(b[...])
        mean = jnp.sum(jnp.sum(sums[which], axis=0, keepdims=True), axis=1, keepdims=True) / entries
        scale = 1.0 / jnp.sqrt(mean + 0.25)
        m, sqr, direction = moments(red[which], f[...], s[...])
        moment[...] = m
        square[...] = sqr
        high = direction.astype(BF)
        low = (direction - high.astype(F32)).astype(BF)
        own = lax.dot_general(high, factor, turn, preferred_element_type=F32)
        own = scale * (own + lax.dot_general(low, factor, turn, preferred_element_type=F32))
        step[...] = own
        new[...] = w[...] - 0.1 * own
        for z in range(N):
            if which == 0:
                rows, codes = d[:, :, z], wall[:, :, z]
            else:
                rows, codes = d[:, z], wall[:, z]
            rows = jnp.stack([rows[0], rows[1]], axis=1).reshape(2 * N * 16, 128)
            codes = jnp.stack([codes[0], codes[1]], axis=1).reshape(2 * N * 16, 256)
            there = lax.dot_general(rows, factor, turn, preferred_element_type=F32)
            copy[z * 256:(z + 1) * 256, :] = (decode(codes) - 0.1 * (scale * there)).astype(BF)


def per_device(x, qc, vc, wq, wv, bq, bv, fq, sq, fv, sv):
    tokens = x.shape[0]
    n_load, n_send = 32, 180
    vmem = pltpu.VMEM
    small_shape = jax.ShapeDtypeStruct
    dq, dv, wall_q, wall_v, red, ss = pl.pallas_call(
        talk,
        out_shape=(
            small_shape((2, N, N, 16, 128), BF), small_shape((2, N, N, 16, 128), BF),
            small_shape((2, N, N, 16, 256), BF), small_shape((2, N, N, 16, 256), BF),
            small_shape((2, 16, 128), F32), small_shape((8, 2, 8, 128), F32),
        ),
        in_specs=[ANY] * 11,
        out_specs=[ANY] * 6,
        scratch_shapes=[
            vmem((N, tokens, 256), BF), vmem((tokens, 256), BF), vmem((tokens, 256), BF),
            vmem((256, RK), BF), vmem((256, RK), BF), vmem((16, 256), F32), vmem((16, 256), F32),
            vmem((4, 16, 128), F32), vmem((tokens, 256), BF),
            vmem((N, 2, N, 16, 128), F32), vmem((N, 2, N, 16, 128), BF), vmem((N, 2, N, 16, 128), BF),
            vmem((N, N, 16, 128), BF), vmem((N, N, 16, 128), BF),
            vmem((N, N, 16, 128), BF), vmem((N, N, 16, 128), BF),
            vmem((N, 16, 128), BF), vmem((N, 16, 128), BF), vmem((N, 16, 128), BF), vmem((N, 16, 128), BF),
            vmem((2, N, N, 16, 128), BF), vmem((2, N, N, 16, 128), BF),
            vmem((2, N, N, 16, 256), BF), vmem((2, N, N, 16, 256), BF),
            vmem((2, 16, 128), F32), vmem((8, 2, 8, 128), F32),
            pltpu.SemaphoreType.DMA((n_load,)), pltpu.SemaphoreType.DMA((n_send,)),
            pltpu.SemaphoreType.DMA((n_send,)),
        ],
        compiler_params=pltpu.CompilerParams(collective_id=0, has_side_effects=True),
    )(x, qc, vc, bq, bv, wq, wv, fq, sq, fv, sv)
    wide, narrow = small_shape((16, 256), F32), small_shape((16, 128), F32)
    whole = small_shape((D, 256), BF)
    return pl.pallas_call(
        finish,
        out_shape=(wide, wide, wide, wide, whole, whole, narrow, narrow, narrow, narrow),
        in_specs=[VM] * 14,
        out_specs=[VM] * 10,
    )(dq, dv, wall_q, wall_v, red, ss, bq, bv, wq, wv, fq, sq, fv, sv)


def solution(mesh):
    return jax.shard_map(
        per_device,
        mesh=mesh,
        in_specs=(
            P("fs", None), P("fs", "tp"), P("fs", "tp"), P("fs", "tp"), P("fs", "tp"),
            P("tp", None), P("tp", None), P("fs", "tp"), P("fs", "tp"), P("fs", "tp"), P("fs", "tp"),
        ),
        out_specs=(
            P("fs", "tp"), P("fs", "tp"), P("fs", "tp"), P("fs", "tp"), P(None, "tp"), P(None, "tp"),
            P("fs", "tp"), P("fs", "tp"), P("fs", "tp"), P("fs", "tp"),
        ),
        check_vma=False,
    )
```

```python
import functools

import jax
import jax.numpy as jnp
from jax import lax
from jax.experimental import pallas as pl
from jax.experimental.pallas import tpu as pltpu
from jax.sharding import PartitionSpec as P

D = 2048
HEADS = 16
HEAD = 64
RK = 32
N = 8
READY = 2
ORDER = (4, 3, 5, 2, 6, 1, 7)
BF = jnp.bfloat16
F32 = jnp.float32
MESH = pl.DeviceIdType.MESH
TURN = (((1,), (1,)), ((), ()))
ANY = pl.BlockSpec(memory_space=pl.ANY)
VM = pl.BlockSpec(memory_space=pltpu.VMEM)


def spread(basis):
    rank, rows = basis.shape
    wide = rows // HEAD * rank
    copies = lax.broadcasted_iota(jnp.int32, (wide, rank), 0) % rank
    pick = (lax.broadcasted_iota(jnp.int32, (wide, rank), 1) == copies).astype(BF)
    tiled = jnp.dot(pick, basis, preferred_element_type=F32)
    row = lax.broadcasted_iota(jnp.int32, (wide, rows), 0) // rank
    col = lax.broadcasted_iota(jnp.int32, (wide, rows), 1) // HEAD
    return jnp.where(row == col, tiled, 0.0).astype(BF)


def moments(reduced, first, second):
    moment = 0.9 * first + 0.1 * reduced
    square = 0.95 * second + 0.05 * reduced * reduced
    direction = moment / (jnp.sqrt(square) + 1e-08)
    return moment, square, direction


def encode(w):
    s = w * w
    return jnp.where(w < 0, -(s * s), s * s).astype(BF)


def decode(code):
    c = code.astype(F32)
    size = lax.rsqrt(lax.rsqrt(jnp.maximum(jnp.abs(c), 1e-30)))
    return jnp.where(c < 0, -size, size)


def talk(
    x_hbm, qc_hbm, vc_hbm, bq_hbm, bv_hbm, wq_hbm, wv_hbm, fq_hbm, sq_hbm, fv_hbm, sv_hbm,
    dq_out, dv_out, wq_out, wv_out, red_out, ss_out,
    x, qc, vc, bq, bv, wq, wv, mom, small, parts, d2d_recv,
    send_q, recv_q, send_v, recv_v, send2_q, recv2_q, send2_v, recv2_v,
    dq, dv, wall_q, wall_v, red, ss, load_sem, ssem, rsem,
):
    fs = lax.axis_index("fs")
    tp = lax.axis_index("tp")
    c = fs % 2
    y = (fs // 2) % N
    z = fs // (2 * N)
    other = fs + 1 - 2 * c

    def on_y(k):
        return {"fs": (z * N + (y + k) % N) * 2 + c}

    def on_z(k):
        return {"fs": (((z + k) % N) * N + y) * 2 + c}

    partner = {"fs": other}
    over_x = [{"fs": f, "tp": (tp + k) % 4} for f, k in
              [(fs, 1), (fs, 2), (fs, 3), (other, 0), (other, 1), (other, 2), (other, 3)]]

    barrier = pltpu.get_barrier_semaphore()
    greeted = [on_y(k) for k in ORDER] + [on_z(k) for k in ORDER] + over_x
    for device in greeted:
        pl.semaphore_signal(barrier, inc=1, device_id=device, device_id_type=MESH)

    loads = []

    def load(src, dst):
        copy = pltpu.make_async_copy(src, dst, load_sem.at[len(loads)])
        copy.start()
        loads.append(copy)
        return copy

    sent = []

    def send(src, dst, device):
        at = len(sent)
        copy = pltpu.make_async_remote_copy(
            src_ref=src, dst_ref=dst, send_sem=ssem.at[at], recv_sem=rsem.at[at],
            device_id=device, device_id_type=MESH)
        copy.start()
        sent.append(copy)
        return copy

    first = [load(bq_hbm, bq), load(bv_hbm, bv), load(qc_hbm, qc), load(vc_hbm, vc)]
    order = ORDER + (0,)
    chunk_z = [(z + k) % N for k in order]
    chunks = [
        load(x_hbm.at[:, pl.ds(pl.multiple_of(chunk_z[j] * 256, 256), 256)], x.at[j]) for j in range(N)
    ]
    later_w = [load(wq_hbm, wq), load(wv_hbm, wv)]
    later_m = [load(r, mom.at[i]) for i, r in enumerate((fq_hbm, sq_hbm, fv_hbm, sv_hbm))]

    for copy in first:
        copy.wait()
    small[:128] = lax.dot_general(spread(bq[...]), qc[...], TURN, preferred_element_type=F32).astype(BF)
    small[128:] = lax.dot_general(spread(bv[...]), vc[...], TURN, preferred_element_type=F32).astype(BF)

    d2d = []

    def product(j):
        chunks[j].wait()
        out = jnp.dot(small[...], x[j], preferred_element_type=F32).astype(BF).T.reshape(N, 2, 16, 256)
        for core in range(2):
            parts[j, core, 0] = out[:, core, :, :128]
            parts[j, core, 1] = out[:, core, :, 128:]
        if j >= READY:
            give(j)

    def give(j):
        d2d.append(send(parts.at[j, 1 - c], d2d_recv.at[j], partner))

    rs1_v = []

    rs1_q = []

    def combine(j):
        d2d[j].wait_recv()
        both = (parts[j, pl.ds(c, 1)][0].astype(F32) + d2d_recv[j].astype(F32)).astype(BF)
        send_q[:, j] = both[0]
        send_v[j] = both[1]
        if order[j] != 0:
            rs1_v.append((order[j], send(send_v.at[j], recv_v.at[order[j]], on_z(order[j]))))
        if j % 2:
            for k in ORDER:
                span = pl.ds(j - 1, 2)
                rs1_q.append((k, j // 2, send(send_q.at[(y + k) % N, span], recv_q.at[k, span], on_y(k))))

    for j in range(READY):
        product(j)
    pl.semaphore_wait(barrier, len(greeted))
    for j in range(READY):
        give(j)

    for copy in later_w:
        copy.wait()
    wall_q[pl.ds(c, 1), pl.ds(y, 1), pl.ds(z, 1)] = encode(wq[...])[None, None, None]
    wall_v[pl.ds(c, 1), pl.ds(z, 1), pl.ds(y, 1)] = encode(wv[...])[None, None, None]
    w1 = []
    for k in ORDER:
        w1.append(send(wall_q.at[c, y, z], wall_q.at[c, y, z], on_z(k)))
        w1.append(send(wall_v.at[c, z, y], wall_v.at[c, z, y], on_y(k)))
    for j in range(READY, N):
        product(j)
        combine(j - READY)
    for j in range(N - READY, N):
        combine(j)

    forwards = []

    def forward(ref, index):
        forwards.append(send(ref.at[c, index], ref.at[c, index], partner))

    for copy in w1:
        copy.wait_recv()
    right, left = [], []

    def w_step(s):
        if s > 0:
            right[-2].wait_recv()
            right[-1].wait_recv()
            forward(wall_q, (y + N - s) % N)
            forward(wall_v, (z + N - s) % N)
            if s < 4:
                left[-2].wait_recv()
                left[-1].wait_recv()
                forward(wall_q, (y + s) % N)
                forward(wall_v, (z + s) % N)
        else:
            forward(wall_q, y)
            forward(wall_v, z)
        if s < 4:
            a, b = (y + N - s) % N, (z + N - s) % N
            right.append(send(wall_q.at[c, a], wall_q.at[c, a], on_y(1)))
            right.append(send(wall_v.at[c, b], wall_v.at[c, b], on_z(1)))
        if s < 3:
            a, b = (y + s) % N, (z + s) % N
            left.append(send(wall_q.at[c, a], wall_q.at[c, a], on_y(N - 1)))
            left.append(send(wall_v.at[c, b], wall_v.at[c, b], on_z(N - 1)))

    w_step(0)

    total_v = send_v[N - 1].astype(F32)
    for k, copy in rs1_v:
        copy.wait_recv()
        total_v = total_v + recv_v[k].astype(F32)
    send2_v[...] = total_v.astype(BF)
    rs2_v = [(k, send(send2_v.at[(y + k) % N], recv2_v.at[k], on_y(k))) for k in ORDER]
    for _, _, copy in rs1_q:
        copy.wait_recv()
    total_q = send_q[pl.ds(y, 1)][0].astype(F32)
    for k in ORDER:
        total_q = total_q + recv_q[k].astype(F32)
    send2_q[...] = total_q.astype(BF)
    rs2_q = [(k, send(send2_q.at[order.index(k)], recv2_q.at[k], on_z(k))) for k in ORDER]
    w_step(1)

    reduced_v = send2_v[pl.ds(y, 1)][0].astype(F32)
    for k, copy in rs2_v:
        copy.wait_recv()
        reduced_v = reduced_v + recv2_v[k].astype(F32)
    reduced_q = send2_q[N - 1].astype(F32)
    for k, copy in rs2_q:
        copy.wait_recv()
        reduced_q = reduced_q + recv2_q[k].astype(F32)
    for copy in later_m:
        copy.wait()
    red[0] = reduced_q
    red[1] = reduced_v
    direction_q = moments(reduced_q, mom[0], mom[1])[2]
    direction_v = moments(reduced_v, mom[2], mom[3])[2]
    dq[pl.ds(c, 1), pl.ds(y, 1), pl.ds(z, 1)] = direction_q.astype(BF)[None, None, None]
    dv[pl.ds(c, 1), pl.ds(z, 1), pl.ds(y, 1)] = direction_v.astype(BF)[None, None, None]
    ag1 = []
    for k in ORDER:
        ag1.append(send(dq.at[c, y, z], dq.at[c, y, z], on_z(k)))
        ag1.append(send(dv.at[c, z, y], dv.at[c, z, y], on_y(k)))
    w_step(2)
    for copy in ag1:
        copy.wait_recv()
    ag2 = []
    for k in ORDER:
        ag2.append((k, send(dq.at[c, y], dq.at[c, y], on_y(k)), send(dv.at[c, z], dv.at[c, z], on_z(k))))
    forward(dq, y)
    forward(dv, z)
    w_step(3)

    def squares(ref, index):
        t = ref[pl.ds(c, 1), pl.ds(index, 1)].astype(F32).reshape(N * 2, 8, 128)
        return jnp.sum(t * t, axis=0)

    ss_q = squares(dq, y)
    ss_v = squares(dv, z)
    for k, copy_q, copy_v in sorted(ag2, key=lambda t: min(t[0], N - t[0])):
        a, b = (y + N - k) % N, (z + N - k) % N
        copy_q.wait_recv()
        forward(dq, a)
        ss_q = ss_q + squares(dq, a)
        copy_v.wait_recv()
        forward(dv, b)
        ss_v = ss_v + squares(dv, b)
    ss[0, 0] = ss_q
    ss[0, 1] = ss_v
    sums = [send(ss.at[0], ss.at[1 + i], device) for i, device in enumerate(over_x)]
    w_step(4)
    for copy in forwards:
        copy.wait_recv()
    at = len(loads)
    outs = [load(dq, dq_out), load(dv, dv_out), load(wall_q, wq_out), load(wall_v, wv_out), load(red, red_out)]
    for copy in sums:
        copy.wait_recv()
    outs.append(load(ss, ss_out))
    for copy in sent:
        copy.wait_send()
    for copy in outs:
        copy.wait()


def finish(
    dq, dv, wall_q, wall_v, red, ss, bq, bv, wq, wv, fq, sq, fv, sv,
    step_q, step_v, new_q, new_v, copy_q, copy_v, moment_q, square_q, moment_v, square_v,
):
    entries = D * HEADS * RK
    sums = jnp.sum(ss[...], axis=0)
    for which, (d, wall, b, w, f, s, step, new, copy, moment, square) in enumerate((
        (dq, wall_q, bq, wq, fq, sq, step_q, new_q, copy_q, moment_q, square_q),
        (dv, wall_v, bv, wv, fv, sv, step_v, new_v, copy_v, moment_v, square_v),
    )):
        factor = spread(b[...])
        mean = jnp.sum(jnp.sum(sums[which], axis=0, keepdims=True), axis=1, keepdims=True) / entries
        scale = 1.0 / jnp.sqrt(mean + 0.25)
        m, sqr, direction = moments(red[which], f[...], s[...])
        moment[...] = m
        square[...] = sqr
        high = direction.astype(BF)
        low = (direction - high.astype(F32)).astype(BF)
        own = jnp.dot(high, factor, preferred_element_type=F32)
        own = scale * (own + jnp.dot(low, factor, preferred_element_type=F32))
        step[...] = own
        new[...] = w[...] - 0.1 * own
        for z in range(N):
            if which == 0:
                rows, codes = d[:, :, z], wall[:, :, z]
            else:
                rows, codes = d[:, z], wall[:, z]
            rows = jnp.stack([rows[0], rows[1]], axis=1).reshape(2 * N * 16, 128)
            codes = jnp.stack([codes[0], codes[1]], axis=1).reshape(2 * N * 16, 256)
            there = jnp.dot(rows, factor, preferred_element_type=F32)
            copy[z * 256:(z + 1) * 256, :] = (decode(codes) - 0.1 * (scale * there)).astype(BF)


def per_device(x, qc, vc, wq, wv, bq, bv, fq, sq, fv, sv):
    tokens = x.shape[0]
    n_load, n_send = 32, 190
    bq, bv = bq.T, bv.T
    vmem = pltpu.VMEM
    small_shape = jax.ShapeDtypeStruct
    dq, dv, wall_q, wall_v, red, ss = pl.pallas_call(
        talk,
        out_shape=(
            small_shape((2, N, N, 16, 128), BF), small_shape((2, N, N, 16, 128), BF),
            small_shape((2, N, N, 16, 256), BF), small_shape((2, N, N, 16, 256), BF),
            small_shape((2, 16, 128), F32), small_shape((8, 2, 8, 128), F32),
        ),
        in_specs=[ANY] * 11,
        out_specs=[ANY] * 6,
        scratch_shapes=[
            vmem((N, tokens, 256), BF), vmem((tokens, 256), BF), vmem((tokens, 256), BF),
            vmem((RK, 256), BF), vmem((RK, 256), BF), vmem((16, 256), F32), vmem((16, 256), F32),
            vmem((4, 16, 128), F32), vmem((256, tokens), BF),
            vmem((N, 2, 2, N, 16, 128), BF), vmem((N, 2, N, 16, 128), BF),
            vmem((N, N, 16, 128), BF), vmem((N, N, 16, 128), BF),
            vmem((N, N, 16, 128), BF), vmem((N, N, 16, 128), BF),
            vmem((N, 16, 128), BF), vmem((N, 16, 128), BF), vmem((N, 16, 128), BF), vmem((N, 16, 128), BF),
            vmem((2, N, N, 16, 128), BF), vmem((2, N, N, 16, 128), BF),
            vmem((2, N, N, 16, 256), BF), vmem((2, N, N, 16, 256), BF),
            vmem((2, 16, 128), F32), vmem((8, 2, 8, 128), F32),
            pltpu.SemaphoreType.DMA((n_load,)), pltpu.SemaphoreType.DMA((n_send,)),
            pltpu.SemaphoreType.DMA((n_send,)),
        ],
        compiler_params=pltpu.CompilerParams(collective_id=0, has_side_effects=True),
    )(x, qc, vc, bq, bv, wq, wv, fq, sq, fv, sv)
    wide, narrow = small_shape((16, 256), F32), small_shape((16, 128), F32)
    whole = small_shape((D, 256), BF)
    return pl.pallas_call(
        finish,
        out_shape=(wide, wide, wide, wide, whole, whole, narrow, narrow, narrow, narrow),
        in_specs=[VM] * 14,
        out_specs=[VM] * 10,
    )(dq, dv, wall_q, wall_v, red, ss, bq, bv, wq, wv, fq, sq, fv, sv)


def solution(mesh):
    return jax.shard_map(
        per_device,
        mesh=mesh,
        in_specs=(
            P("fs", None), P("fs", "tp"), P("fs", "tp"), P("fs", "tp"), P("fs", "tp"),
            P("tp", None), P("tp", None), P("fs", "tp"), P("fs", "tp"), P("fs", "tp"), P("fs", "tp"),
        ),
        out_specs=(
            P("fs", "tp"), P("fs", "tp"), P("fs", "tp"), P("fs", "tp"), P(None, "tp"), P(None, "tp"),
            P("fs", "tp"), P("fs", "tp"), P("fs", "tp"), P("fs", "tp"),
        ),
        check_vma=False,
    )
```
